32 devices in a mesh: ep: 8 (over z, y), tp: 4 (over x, core).
Axes of the slice: x: 2, y: 2, z: 4, core: 2. Of those that a mesh axis runs over, the one named last changes fastest.
Arguments:
- tokens: bfloat16 [4096, 2048], P(('ep', 'tp')), may hold values from -6 to 6
- norm_gain: float32 [2048], replicated, may hold values from 0.1 to 1.9
- w_gate: bfloat16 [32, 2048, 512], P(('ep', 'tp')), may hold values from -0.125 to 0.125
- w_up: bfloat16 [32, 2048, 512], P(('ep', 'tp')), may hold values from -0.125 to 0.125
- w_down: bfloat16 [32, 512, 2048], P(('ep', 'tp')), may hold values from -0.25 to 0.25
- routing: int32 [4096, 2], P(('ep', 'tp')), may hold values from 0 to 31, as said below
- gate_weight: float32 [4096, 2], P(('ep', 'tp')), may hold values from 0.05 to 1
Outputs:
- combined: bfloat16 [4096, 2048], P(('ep', 'tp'))
The draws below stay inside these ranges and needn't reach their ends.
Inputs may be any that keep to these rules, and one draw needn't show every extreme that they name: `routing`: A token's 2 experts are distinct and lie in one group of 4 consecutive experts. Of the 128 tokens of each device exactly 16 choose each group; no expert is named by more than 16 tokens of one device, and in every group one expert is named by exactly 16 tokens of every device.
All inputs are finite; a program needn't handle non-finite values.
Results may differ from the reference program's by a relative error of at most 0.0085.
Values may be sent and summed in bfloat16 or wider, within the bound.
A program may use at most 64 MiB of HBM per device.

```python
import math
import jax
import jax.numpy as jnp
from jax import lax

D = 2048
FF = 512
GROUP_EXPERTS = 4
TOP = 2
TOK_DEV = 128
EXPERTS = 32
GROUPS = 8
CAP = 16
TOKENS = 4096


def draw_routing(key, part):
    source_count = TOKENS // TOK_DEV
    heavy_key = jax.random.fold_in(key, 11)
    cut_key = jax.random.fold_in(key, 12)
    shuffle_key = jax.random.fold_in(key, 13)
    heavy_member = jax.random.randint(heavy_key, (GROUPS,), 0, GROUP_EXPERTS)
    cut_points = jax.random.randint(cut_key, (source_count, GROUPS, 2), 0, CAP + 1)
    lower = jnp.min(cut_points, axis=-1)
    higher = jnp.max(cut_points, axis=-1)
    rest_loads = jnp.stack([lower, higher - lower, CAP - higher], axis=-1)
    members = jnp.arange(GROUP_EXPERTS, dtype=jnp.int32)
    is_heavy = members[None, :] == heavy_member[:, None]
    rank = jnp.clip(members[None, :] - (members[None, :] > heavy_member[:, None]).astype(jnp.int32), 0, 2)
    rank_full = jnp.broadcast_to(rank[None], (source_count, GROUPS, GROUP_EXPERTS))
    load_table = jnp.where(is_heavy[None], CAP, jnp.take_along_axis(rest_loads, rank_full, axis=2))
    bounds = jnp.cumsum(load_table, axis=-1)
    entries = jnp.arange(2 * CAP, dtype=jnp.int32)
    local_ident = jnp.sum((entries[None, None, :, None] >= bounds[:, :, None, :GROUP_EXPERTS - 1]).astype(jnp.int32), axis=-1)
    group_base = jnp.arange(GROUPS, dtype=jnp.int32) * GROUP_EXPERTS
    pair_table = jnp.stack([local_ident[:, :, :CAP], local_ident[:, :, CAP:]], axis=-1) + group_base[None, :, None, None]
    pair_table = pair_table.reshape(source_count, TOK_DEV, TOP)
    shuffles = jax.vmap(lambda subkey: jax.random.permutation(subkey, TOK_DEV))(jax.random.split(shuffle_key, source_count))
    routing = jnp.take_along_axis(pair_table, shuffles[:, :, None].astype(jnp.int32), axis=1)
    return routing.reshape(TOKENS, TOP).astype(jnp.int32)


def level_of(rng, shape, shards, low, top_value):
    level, own = 1.0, jax.random.fold_in(rng, 6)
    for dim, blocks in shards:
        steps = jnp.exp(jax.random.uniform(jax.random.fold_in(own, dim), (blocks,), jnp.float32, low / len(shards), top_value / len(shards)))
        level = level * jnp.repeat(steps, shape[dim] // blocks).reshape([-1 if axis == dim else 1 for axis in range(len(shape))])
    return level


def gaussian(rng, shape, spread, most, cuts=(), kind=jnp.bfloat16):
    values = spread * jax.random.normal(rng, shape, jnp.float32)
    if cuts:
        values = values * level_of(rng, shape, cuts, -0.22, 0.18)
    return jnp.clip(values, -most, most).astype(kind)


def setup_inputs(seed: int = 0) -> dict:
    key_list = jax.random.split(jax.random.key(seed), 8)
    tokens = gaussian(key_list[0], (TOKENS, D), 1.0, 6.0, ((0, 32),))
    norm_gain = jnp.clip(1.0 + 0.18 * jax.random.normal(key_list[1], (D,), jnp.float32), 0.1, 1.9)
    w_gate = gaussian(key_list[2], (EXPERTS, D, FF), D ** -0.5, 0.125, ((0, 32),))
    w_up = gaussian(key_list[3], (EXPERTS, D, FF), D ** -0.5, 0.125, ((0, 32),))
    w_down = gaussian(key_list[4], (EXPERTS, FF, D), FF ** -0.5, 0.25, ((0, 32),))
    routing = draw_routing(jax.random.fold_in(key_list[7], 71), 0)
    gate_weight = jnp.clip(jnp.exp(math.log(1.0) - 2.9957323 * jax.random.uniform(key_list[6], (TOKENS, TOP), jnp.float32) ** level_of(key_list[6], (TOKENS, TOP), ((0, 32),), -0.2, 0.2)), 0.05, 1.0)
    return {"tokens": tokens, "norm_gain": norm_gain, "w_gate": w_gate, "w_up": w_up, "w_down": w_down, "routing": routing, "gate_weight": gate_weight}


def reference(tokens, norm_gain, w_gate, w_up, w_down, routing, gate_weight):
    source_count = TOKENS // TOK_DEV
    values = tokens.astype(jnp.float32)
    scale = lax.rsqrt(lax.optimization_barrier(jnp.mean(values * values, axis=-1, keepdims=True)) + 1e-06)
    normed = (values * scale * norm_gain.astype(jnp.float32)).astype(jnp.bfloat16)
    assigned = routing.reshape(source_count, TOK_DEV * TOP).astype(jnp.int32)

    def count_slots(block):
        onehot = (block[:, None] == jnp.arange(EXPERTS, dtype=jnp.int32)[None, :]).astype(jnp.int32)
        running = jnp.cumsum(onehot, axis=0)
        return lax.optimization_barrier(jnp.sum(onehot * running, axis=1)) - 1
    slot_index = lax.map(count_slots, assigned)
    source_index = jnp.arange(source_count, dtype=jnp.int32)[:, None]
    position = (assigned * source_count + source_index) * CAP + slot_index
    dump_index = TOKENS * TOP
    slot_owner = jnp.full((EXPERTS * source_count * CAP,), dump_index, jnp.int32)
    slot_owner = slot_owner.at[position.reshape(-1)].set(jnp.arange(TOKENS * TOP, dtype=jnp.int32))
    slot_owner = slot_owner.reshape(EXPERTS, source_count * CAP)
    normed_pad = jnp.concatenate([normed, jnp.zeros((1, D), jnp.bfloat16)], axis=0)

    def one_expert(expert, results):
        owners = lax.dynamic_index_in_dim(slot_owner, expert, 0, keepdims=False)
        slot_rows = normed_pad[owners // TOP]
        gate_part = jnp.dot(slot_rows, lax.dynamic_index_in_dim(w_gate, expert, 0, keepdims=False), preferred_element_type=jnp.float32)
        up_part = jnp.dot(slot_rows, lax.dynamic_index_in_dim(w_up, expert, 0, keepdims=False), preferred_element_type=jnp.float32)
        hidden = (jax.nn.silu(gate_part) * up_part).astype(jnp.bfloat16)
        expert_out = jnp.dot(hidden, lax.dynamic_index_in_dim(w_down, expert, 0, keepdims=False), preferred_element_type=jnp.float32).astype(jnp.bfloat16)
        return results.at[owners].set(expert_out)
    results = lax.fori_loop(0, EXPERTS, one_expert, jnp.zeros((TOKENS * TOP + 1, D), jnp.bfloat16))
    picked = results[:TOKENS * TOP].reshape(TOKENS, TOP, D).astype(jnp.float32)
    return lax.optimization_barrier(jnp.sum(gate_weight.astype(jnp.float32)[:, :, None] * picked, axis=1)).astype(jnp.bfloat16)
```

```python
import functools
import jax
import jax.numpy as jnp
from jax import lax
from jax.experimental import pallas as pl
from jax.experimental.pallas import tpu as pltpu
from jax.sharding import PartitionSpec as P

BF = jnp.bfloat16
F32 = jnp.float32
MESH = pl.DeviceIdType.MESH

CHUNKS = ((0, 1), (2, 3), (4, 5), (6, 7))
ORDER = (
    "S0 S1 F0 S2",
    "S3 F1 S4 C0",
    "F2 F3 S5 C1",
    "F4 S6 F5 S7",
    "C2 J2 J1 F6",
    "F7 C3 G4 G5",
    "J3 J0 G2 G3",
    "G6 G7",
)
DIRECT = 2
RDIRECT = 2
SENDS = (
    "P1 X1 P2 P3",
    "P4 P5 P6 P7",
)


def flip(index, bits):
    unit = 1
    while unit <= bits:
        if bits & unit:
            index = index + unit - 2 * unit * lax.rem(lax.div(index, unit), 2)
        unit *= 2
    return index


def kernel(
    ep_count, tp_count, block,
    tok_ref, gain_ref, route_ref, gate_ref, wg_hbm, wu_hbm, wd_hbm, out_ref,
    wg, wu, wd, normed, pack, rows_in, hid, part, pair_in, cross_out, cross_in, done, back, back_x,
    w_sem, disp_s, disp_r, core_s, core_r, x_s, x_r, fwd_s, fwd_r,
    pair_s, pair_r, cross_s, cross_r, ret_s, ret_r, rx_s, rx_r,
):
    toks, width = tok_ref.shape
    ff = wg.shape[1]
    slots = ep_count * block
    unit = ep_count // 8
    me_e = lax.axis_index("ep")
    me_t = lax.axis_index("tp")
    partner = {"tp": flip(me_t, 1)}
    across = {"tp": flip(me_t, 2)}
    peer = [{"ep": flip(me_e, d)} for d in range(ep_count)]
    direct, r_direct = DIRECT * unit, RDIRECT * unit
    far_side = [across] + [
        {"ep": flip(me_e, d), "tp": flip(me_t, 2)} for d in range(1, max(direct, r_direct))
    ]

    w_copies = [
        pltpu.make_async_copy(src.at[0], dst, w_sem.at[i])
        for i, (src, dst) in enumerate(((wg_hbm, wg), (wu_hbm, wu), (wd_hbm, wd)))
    ]
    barrier = pltpu.get_barrier_semaphore()
    others = peer[1:] + [partner] + far_side
    for dev in others:
        pl.semaphore_signal(barrier, inc=1, device_id=dev, device_id_type=MESH)
    for c in w_copies:
        c.start()

    values = tok_ref[...].astype(F32)
    scale = lax.rsqrt(jnp.mean(values * values, axis=-1, keepdims=True) + 1e-06)
    normed[...] = (values * scale * gain_ref[...]).astype(BF)

    shift = tp_count.bit_length() - 1
    group = jnp.bitwise_xor(jnp.right_shift(route_ref[0:1, :], shift), me_e)
    in_group = (group == lax.broadcasted_iota(jnp.int32, (ep_count, toks), 0)).astype(F32)
    before = lax.broadcasted_iota(jnp.int32, (toks, toks), 0) < lax.broadcasted_iota(
        jnp.int32, (toks, toks), 1
    )
    ranks = jnp.dot(
        in_group.astype(BF), before.astype(F32).astype(BF), preferred_element_type=F32
    )
    rank = jnp.sum(ranks * in_group, axis=0, keepdims=True).astype(jnp.int32)
    slot = group * block + rank
    packing = slot == lax.broadcasted_iota(jnp.int32, (slots, toks), 0)
    packs = packing.astype(F32).astype(BF)
    step = min(slots, 128)
    for s in range(0, slots, step):
        pack[s : s + step, :width] = jnp.dot(
            packs[s : s + step, :], normed[...], preferred_element_type=F32
        ).astype(BF)
    lane = lax.broadcasted_iota(jnp.int32, (slots, 128), 1)
    weight = jnp.zeros((slots, 128), F32)
    for j in range(tp_count):
        one = jnp.zeros((1, toks), F32)
        for k in range(route_ref.shape[0]):
            hit = jnp.bitwise_and(route_ref[k : k + 1, :], tp_count - 1) == j
            one = one + jnp.where(hit, gate_ref[k : k + 1, :], 0.0)
        picked = jnp.sum(jnp.where(packing, one, 0.0), axis=-1, keepdims=True)
        weight = jnp.where(jnp.bitwise_and(lane, tp_count - 1) == j, picked, weight)
    hi = weight.astype(BF).astype(F32)
    mid = (weight - hi).astype(BF).astype(F32)
    low = weight - hi - mid
    tail = jnp.where(lane < tp_count, hi, jnp.where(lane < 2 * tp_count, mid, low))
    pack[:, width:] = jnp.where(lane < 3 * tp_count, tail, 0.0).astype(BF)

    def remote(src, dst, s, r, dev):
        return pltpu.make_async_remote_copy(
            src_ref=src, dst_ref=dst, send_sem=s, recv_sem=r, device_id=dev, device_id_type=MESH
        )

    chunk_of = {}
    first, count, base = [], [], []
    for k, units in enumerate(CHUNKS):
        first.append(units[0] * unit)
        count.append(len(units) * unit)
        base.append(units[0] * unit * block)
        for d in range(first[k], first[k] + count[k]):
            chunk_of[d] = k

    def place(d, pos):
        k = chunk_of[d]
        seg = count[k] * block
        return rows_in.at[pl.ds(tp_count * base[k] + pos * seg + (d - first[k]) * block, block)]

    rows_in[0:block, :] = pack[0:block, :]
    pl.semaphore_wait(barrier, len(others))

    disp, core, xs, fwd, ret, ret_x, pair, cross = ({} for _ in range(8))

    def send_peer(d):
        disp[d] = remote(
            pack.at[pl.ds(d * block, block)], place(d, 0), disp_s.at[d], disp_r.at[d], peer[d]
        )
        disp[d].start()

    def send_across(d, dev):
        src = pack.at[pl.ds(d * block, block)] if d < direct else place(d, 0)
        xs[d] = remote(src, place(d, 1), x_s.at[d], x_r.at[d], dev)
        xs[d].start()

    def send_core(d):
        core[d] = remote(place(d, 0), place(d, 2), core_s.at[d], core_r.at[d], partner)
        core[d].start()

    send_across(0, across)
    send_core(0)
    for d in range(1, unit):
        send_peer(d)
        send_across(d, far_side[d])
    for word in " ".join(SENDS).split():
        i = int(word[1:])
        for d in range(i * unit, i * unit + unit):
            if word[0] == "P":
                send_peer(d)
            else:
                send_across(d, far_side[d])

    def spread(i):
        for d in range(i * unit, i * unit + unit):
            if d > 0:
                disp[d].wait_recv()
                if d >= direct:
                    send_across(d, across)
                send_core(d)

    def forward(i):
        for d in range(i * unit, i * unit + unit):
            xs[d].wait_recv()
            fwd[d] = remote(place(d, 1), place(d, 3), fwd_s.at[d], fwd_r.at[d], partner)
            fwd[d].start()

    def compute(k):
        for d in range(first[k], first[k] + count[k]):
            core[d].wait_recv()
            fwd[d].wait_recv()
        if k == 0:
            for c in w_copies:
                c.wait()
        seg = count[k] * block
        total = tp_count * seg
        mine = pl.ds(tp_count * base[k], total)
        ends = lax.broadcasted_iota(jnp.int32, (total, 128), 1)
        own = jnp.bitwise_and(ends, tp_count - 1) == me_t
        gates = jnp.sum(
            jnp.where(own, rows_in[mine, width:].astype(F32), 0.0), axis=-1, keepdims=True
        )
        f_tile = min(ff, 256)
        for j in range(0, ff, f_tile):
            rows = rows_in[mine, :width]
            g = jnp.dot(rows, wg[:, j : j + f_tile], preferred_element_type=F32)
            u = jnp.dot(rows, wu[:, j : j + f_tile], preferred_element_type=F32)
            hid[0:total, j : j + f_tile] = (g / (1.0 + jnp.exp(-g)) * u).astype(BF)
        d_tile = min(width, 512)
        for j in range(0, width, d_tile):
            y = jnp.dot(hid[0:total, :], wd[:, j : j + d_tile], preferred_element_type=F32)
            part[mine, j : j + d_tile] = (y * gates).astype(BF)
        pair[k] = remote(
            part.at[pl.ds(tp_count * base[k] + 2 * seg, 2 * seg)],
            pair_in.at[pl.ds(2 * base[k], 2 * seg)], pair_s.at[k], pair_r.at[k], partner,
        )
        pair[k].start()

    def give_block(d):
        ret[d] = remote(
            done.at[pl.ds(d * block, block)], back.at[pl.ds(d * block, block)],
            ret_s.at[d], ret_r.at[d], peer[d],
        )
        ret[d].start()

    def join(k):
        pair[k].wait_recv()
        seg = count[k] * block
        b, p = base[k], tp_count * base[k]
        cross_out[b : b + seg, :] = (
            part[p + seg : p + 2 * seg, :].astype(F32)
            + pair_in[2 * b + seg : 2 * b + 2 * seg, :].astype(F32)
        ).astype(BF)
        if first[k] >= r_direct:
            for d in range(first[k], first[k] + count[k]):
                cross[d] = remote(
                    cross_out.at[pl.ds(d * block, block)], cross_in.at[pl.ds(d * block, block)],
                    cross_s.at[d], cross_r.at[d], across,
                )
                cross[d].start()
            return
        for d in range(first[k], first[k] + count[k]):
            ret_x[d] = remote(
                cross_out.at[pl.ds(d * block, block)], back_x.at[pl.ds(d * block, block)],
                rx_s.at[d], rx_r.at[d], far_side[d],
            )
            ret_x[d].start()
        total = (
            part[p : p + seg, :].astype(F32) + pair_in[2 * b : 2 * b + seg, :].astype(F32)
        ).astype(BF)
        done[b : b + seg, :] = total
        for d in range(first[k], first[k] + count[k]):
            if d == 0:
                back[0:block, :] = total[0:block, :]
            else:
                give_block(d)

    def give(i):
        for d in range(i * unit, i * unit + unit):
            cross[d].wait_recv()
            k = chunk_of[d]
            b, p = d * block, tp_count * base[k] + (d - first[k]) * block
            q = 2 * base[k] + (d - first[k]) * block
            done[b : b + block, :] = (
                part[p : p + block, :].astype(F32)
                + pair_in[q : q + block, :].astype(F32)
                + cross_in[b : b + block, :].astype(F32)
            ).astype(BF)
            give_block(d)

    step_of = {"S": spread, "F": forward, "C": compute, "J": join, "G": give}
    for word in " ".join(ORDER).split():
        step_of[word[0]](int(word[1:]))

    for d in sorted(ret):
        ret[d].wait_recv()
    for d in sorted(ret_x):
        ret_x[d].wait_recv()
    unpack = packing.astype(F32).T.astype(BF)
    total = jnp.dot(unpack, back[...], preferred_element_type=F32)
    total = total + jnp.dot(
        unpack[:, : r_direct * block], back_x[...], preferred_element_type=F32
    )
    out_ref[...] = total.astype(BF)
    for group_of in (disp, core, xs, fwd, pair, cross, ret, ret_x):
        for c in group_of.values():
            c.wait_send()


def local(tokens, norm_gain, w_gate, w_up, w_down, routing, gate_weight):
    toks, width = tokens.shape
    ff = w_gate.shape[2]
    ep_count = lax.axis_size("ep")
    tp_count = lax.axis_size("tp")
    assert tp_count == 4 and ep_count % 8 == 0
    cap = toks // ep_count
    block = -(-cap // 16) * 16
    slots = ep_count * block
    wide = width + 128
    most = tp_count * block * (ep_count // 8) * max(len(units) for units in CHUNKS)
    vm = pl.BlockSpec(memory_space=pltpu.VMEM)
    hbm = pl.BlockSpec(memory_space=pl.ANY)
    dma = pltpu.SemaphoreType.DMA
    n_sem = [3] + [ep_count] * 8 + [len(CHUNKS)] * 2 + [ep_count] * 6
    return pl.pallas_call(
        functools.partial(kernel, ep_count, tp_count, block),
        out_shape=jax.ShapeDtypeStruct((toks, width), BF),
        in_specs=[vm] * 4 + [hbm] * 3,
        out_specs=vm,
        scratch_shapes=[
            pltpu.VMEM((width, ff), BF),
            pltpu.VMEM((width, ff), BF),
            pltpu.VMEM((ff, width), BF),
            pltpu.VMEM((toks, width), BF),
            pltpu.VMEM((slots, wide), BF),
            pltpu.VMEM((tp_count * slots, wide), BF),
            pltpu.VMEM((most, ff), BF),
            pltpu.VMEM((tp_count * slots, width), BF),
            pltpu.VMEM((2 * slots, width), BF),
            pltpu.VMEM((slots, width), BF),
            pltpu.VMEM((slots, width), BF),
            pltpu.VMEM((slots, width), BF),
            pltpu.VMEM((slots, width), BF),
            pltpu.VMEM((RDIRECT * slots // 8, width), BF),
        ] + [dma((n,)) for n in n_sem],
        compiler_params=pltpu.CompilerParams(
            collective_id=0, has_side_effects=True, vmem_limit_bytes=60 * 1024 * 1024
        ),
    )(tokens, norm_gain.reshape(1, width), routing.T, gate_weight.T, w_gate, w_up, w_down)


def solution(mesh):
    placed = (
        P(("ep", "tp"), None),
        P(),
        P(("ep", "tp"), None, None),
        P(("ep", "tp"), None, None),
        P(("ep", "tp"), None, None),
        P(("ep", "tp"), None),
        P(("ep", "tp"), None),
    )
    return jax.shard_map(
        local, mesh=mesh, in_specs=placed, out_specs=P(("ep", "tp"), None), check_vma=False
    )
```

```python
import functools
import jax
import jax.numpy as jnp
from jax import lax
from jax.experimental import pallas as pl
from jax.experimental.pallas import tpu as pltpu
from jax.sharding import PartitionSpec as P

BF = jnp.bfloat16
F32 = jnp.float32
MESH = pl.DeviceIdType.MESH

CHUNKS = ((0, 1), (2, 3), (4,), (5,), (6,), (7,))
ORDER = (
    "S0 F0 S4 S2",
    "S3 F4 S5 C2",
    "F2 F3 S7 F5",
    "C1 S1 J2 F1",
    "C3 S6 F7 J3",
    "C5 G4 J1 F6",
    "C4 J5 G5 C0",
    "G3 J4 G7 J0",
    "G6 G2",
)
DIRECT = 2
RDIRECT = 2
SENDS = (
    "P2 P4 P1 P3",
    "P5 P7 X1 P6",
)


def flip(index, bits):
    unit = 1
    while unit <= bits:
        if bits & unit:
            index = index + unit - 2 * unit * lax.rem(lax.div(index, unit), 2)
        unit *= 2
    return index


def kernel(
    ep_count, tp_count, block,
    tok_ref, gain_ref, route_ref, gate_ref, wg_hbm, wu_hbm, wd_hbm, out_ref,
    wg, wu, wd, normed, pack, rows_in, hid, part, pair_in, cross_out, cross_in, done, back, back_x,
    w_sem, disp_s, disp_r, core_s, core_r, x_s, x_r, fwd_s, fwd_r,
    pair_s, pair_r, cross_s, cross_r, ret_s, ret_r, rx_s, rx_r,
):
    toks, width = tok_ref.shape
    ff = wg.shape[1]
    slots = ep_count * block
    unit = ep_count // 8
    me_e = lax.axis_index("ep")
    me_t = lax.axis_index("tp")
    partner = {"tp": flip(me_t, 1)}
    across = {"tp": flip(me_t, 2)}
    peer = [{"ep": flip(me_e, d)} for d in range(ep_count)]
    direct, r_direct = DIRECT * unit, RDIRECT * unit
    far_side = [across] + [
        {"ep": flip(me_e, d), "tp": flip(me_t, 2)} for d in range(1, max(direct, r_direct))
    ]

    w_copies = [
        pltpu.make_async_copy(src.at[0], dst, w_sem.at[i])
        for i, (src, dst) in enumerate(((wg_hbm, wg), (wu_hbm, wu), (wd_hbm, wd)))
    ]
    barrier = pltpu.get_barrier_semaphore()
    others = peer[1:] + [partner] + far_side
    for dev in others:
        pl.semaphore_signal(barrier, inc=1, device_id=dev, device_id_type=MESH)
    for c in w_copies:
        c.start()

    values = tok_ref[...].astype(F32)
    scale = lax.rsqrt(jnp.mean(values * values, axis=-1, keepdims=True) + 1e-06)
    normed[...] = (values * scale * gain_ref[...]).astype(BF)

    shift = tp_count.bit_length() - 1
    group = jnp.bitwise_xor(jnp.right_shift(route_ref[0:1, :], shift), me_e)
    in_group = (group == lax.broadcasted_iota(jnp.int32, (ep_count, toks), 0)).astype(F32)
    before = lax.broadcasted_iota(jnp.int32, (toks, toks), 0) < lax.broadcasted_iota(
        jnp.int32, (toks, toks), 1
    )
    ranks = jnp.dot(
        in_group.astype(BF), before.astype(F32).astype(BF), preferred_element_type=F32
    )
    rank = jnp.sum(ranks * in_group, axis=0, keepdims=True).astype(jnp.int32)
    slot = group * block + rank
    packing = slot == lax.broadcasted_iota(jnp.int32, (slots, toks), 0)
    packs = packing.astype(F32).astype(BF)
    step = min(slots, 128)
    for s in range(0, slots, step):
        pack[s : s + step, :width] = jnp.dot(
            packs[s : s + step, :], normed[...], preferred_element_type=F32
        ).astype(BF)
    lane = lax.broadcasted_iota(jnp.int32, (slots, 128), 1)
    weight = jnp.zeros((slots, 128), F32)
    for j in range(tp_count):
        one = jnp.zeros((1, toks), F32)
        for k in range(route_ref.shape[0]):
            hit = jnp.bitwise_and(route_ref[k : k + 1, :], tp_count - 1) == j
            one = one + jnp.where(hit, gate_ref[k : k + 1, :], 0.0)
        picked = jnp.sum(jnp.where(packing, one, 0.0), axis=-1, keepdims=True)
        weight = jnp.where(jnp.bitwise_and(lane, tp_count - 1) == j, picked, weight)
    hi = weight.astype(BF).astype(F32)
    mid = (weight - hi).astype(BF).astype(F32)
    low = weight - hi - mid
    tail = jnp.where(lane < tp_count, hi, jnp.where(lane < 2 * tp_count, mid, low))
    pack[:, width:] = jnp.where(lane < 3 * tp_count, tail, 0.0).astype(BF)

    def remote(src, dst, s, r, dev):
        return pltpu.make_async_remote_copy(
            src_ref=src, dst_ref=dst, send_sem=s, recv_sem=r, device_id=dev, device_id_type=MESH
        )

    chunk_of = {}
    first, count, base = [], [], []
    for k, units in enumerate(CHUNKS):
        first.append(units[0] * unit)
        count.append(len(units) * unit)
        base.append(units[0] * unit * block)
        for d in range(first[k], first[k] + count[k]):
            chunk_of[d] = k

    def place(d, pos):
        k = chunk_of[d]
        seg = count[k] * block
        return rows_in.at[pl.ds(tp_count * base[k] + pos * seg + (d - first[k]) * block, block)]

    rows_in[0:block, :] = pack[0:block, :]
    pl.semaphore_wait(barrier, len(others))

    disp, core, xs, fwd, ret, ret_x, pair, cross = ({} for _ in range(8))

    def send_peer(d):
        disp[d] = remote(
            pack.at[pl.ds(d * block, block)], place(d, 0), disp_s.at[d], disp_r.at[d], peer[d]
        )
        disp[d].start()

    def send_across(d, dev):
        src = pack.at[pl.ds(d * block, block)] if d < direct else place(d, 0)
        xs[d] = remote(src, place(d, 1), x_s.at[d], x_r.at[d], dev)
        xs[d].start()

    def send_core(d):
        core[d] = remote(place(d, 0), place(d, 2), core_s.at[d], core_r.at[d], partner)
        core[d].start()

    send_across(0, across)
    send_core(0)
    for d in range(1, unit):
        send_peer(d)
        send_across(d, far_side[d])
    for word in " ".join(SENDS).split():
        i = int(word[1:])
        for d in range(i * unit, i * unit + unit):
            if word[0] == "P":
                send_peer(d)
            else:
                send_across(d, far_side[d])

    def spread(i):
        for d in range(i * unit, i * unit + unit):
            if d > 0:
                disp[d].wait_recv()
                if d >= direct:
                    send_across(d, across)
                send_core(d)

    def forward(i):
        for d in range(i * unit, i * unit + unit):
            xs[d].wait_recv()
            fwd[d] = remote(place(d, 1), place(d, 3), fwd_s.at[d], fwd_r.at[d], partner)
            fwd[d].start()

    def compute(k):
        for d in range(first[k], first[k] + count[k]):
            core[d].wait_recv()
            fwd[d].wait_recv()
        if not pair:
            for c in w_copies:
                c.wait()
        seg = count[k] * block
        total = tp_count * seg
        mine = pl.ds(tp_count * base[k], total)
        ends = lax.broadcasted_iota(jnp.int32, (total, 128), 1)
        own = jnp.bitwise_and(ends, tp_count - 1) == me_t
        gates = jnp.sum(
            jnp.where(own, rows_in[mine, width:].astype(F32), 0.0), axis=-1, keepdims=True
        )
        f_tile = min(ff, 256)
        for j in range(0, ff, f_tile):
            rows = rows_in[mine, :width]
            g = jnp.dot(rows, wg[:, j : j + f_tile], preferred_element_type=F32)
            u = jnp.dot(rows, wu[:, j : j + f_tile], preferred_element_type=F32)
            hid[0:total, j : j + f_tile] = (g / (1.0 + jnp.exp(-g)) * u).astype(BF)
        d_tile = min(width, 512)
        for j in range(0, width, d_tile):
            y = jnp.dot(hid[0:total, :], wd[:, j : j + d_tile], preferred_element_type=F32)
            part[mine, j : j + d_tile] = (y * gates).astype(BF)
        pair[k] = remote(
            part.at[pl.ds(tp_count * base[k] + 2 * seg, 2 * seg)],
            pair_in.at[pl.ds(2 * base[k], 2 * seg)], pair_s.at[k], pair_r.at[k], partner,
        )
        pair[k].start()

    def give_block(d):
        ret[d] = remote(
            done.at[pl.ds(d * block, block)], back.at[pl.ds(d * block, block)],
            ret_s.at[d], ret_r.at[d], peer[d],
        )
        ret[d].start()

    def join(k):
        pair[k].wait_recv()
        seg = count[k] * block
        b, p = base[k], tp_count * base[k]
        cross_out[b : b + seg, :] = (
            part[p + seg : p + 2 * seg, :].astype(F32)
            + pair_in[2 * b + seg : 2 * b + 2 * seg, :].astype(F32)
        ).astype(BF)
        if first[k] >= r_direct:
            for d in range(first[k], first[k] + count[k]):
                cross[d] = remote(
                    cross_out.at[pl.ds(d * block, block)], cross_in.at[pl.ds(d * block, block)],
                    cross_s.at[d], cross_r.at[d], across,
                )
                cross[d].start()
            return
        for d in range(first[k], first[k] + count[k]):
            ret_x[d] = remote(
                cross_out.at[pl.ds(d * block, block)], back_x.at[pl.ds(d * block, block)],
                rx_s.at[d], rx_r.at[d], far_side[d],
            )
            ret_x[d].start()
        total = (
            part[p : p + seg, :].astype(F32) + pair_in[2 * b : 2 * b + seg, :].astype(F32)
        ).astype(BF)
        done[b : b + seg, :] = total
        for d in range(first[k], first[k] + count[k]):
            if d == 0:
                back[0:block, :] = total[0:block, :]
            else:
                give_block(d)

    def give(i):
        for d in range(i * unit, i * unit + unit):
            cross[d].wait_recv()
            k = chunk_of[d]
            b, p = d * block, tp_count * base[k] + (d - first[k]) * block
            q = 2 * base[k] + (d - first[k]) * block
            done[b : b + block, :] = (
                part[p : p + block, :].astype(F32)
                + pair_in[q : q + block, :].astype(F32)
                + cross_in[b : b + block, :].astype(F32)
            ).astype(BF)
            give_block(d)

    step_of = {"S": spread, "F": forward, "C": compute, "J": join, "G": give}
    for word in " ".join(ORDER).split():
        step_of[word[0]](int(word[1:]))

    for d in sorted(ret):
        ret[d].wait_recv()
    for d in sorted(ret_x):
        ret_x[d].wait_recv()
    unpack = packing.astype(F32).T.astype(BF)
    total = jnp.dot(unpack, back[...], preferred_element_type=F32)
    total = total + jnp.dot(
        unpack[:, : r_direct * block], back_x[...], preferred_element_type=F32
    )
    out_ref[...] = total.astype(BF)
    for group_of in (disp, core, xs, fwd, pair, cross, ret, ret_x):
        for c in group_of.values():
            c.wait_send()


def local(tokens, norm_gain, w_gate, w_up, w_down, routing, gate_weight):
    toks, width = tokens.shape
    ff = w_gate.shape[2]
    ep_count = lax.axis_size("ep")
    tp_count = lax.axis_size("tp")
    assert tp_count == 4 and ep_count % 8 == 0
    cap = toks // ep_count
    block = -(-cap // 16) * 16
    slots = ep_count * block
    wide = width + 128
    most = tp_count * block * (ep_count // 8) * max(len(units) for units in CHUNKS)
    vm = pl.BlockSpec(memory_space=pltpu.VMEM)
    hbm = pl.BlockSpec(memory_space=pl.ANY)
    dma = pltpu.SemaphoreType.DMA
    n_sem = [3] + [ep_count] * 8 + [len(CHUNKS)] * 2 + [ep_count] * 6
    return pl.pallas_call(
        functools.partial(kernel, ep_count, tp_count, block),
        out_shape=jax.ShapeDtypeStruct((toks, width), BF),
        in_specs=[vm] * 4 + [hbm] * 3,
        out_specs=vm,
        scratch_shapes=[
            pltpu.VMEM((width, ff), BF),
            pltpu.VMEM((width, ff), BF),
            pltpu.VMEM((ff, width), BF),
            pltpu.VMEM((toks, width), BF),
            pltpu.VMEM((slots, wide), BF),
            pltpu.VMEM((tp_count * slots, wide), BF),
            pltpu.VMEM((most, ff), BF),
            pltpu.VMEM((tp_count * slots, width), BF),
            pltpu.VMEM((2 * slots, width), BF),
            pltpu.VMEM((slots, width), BF),
            pltpu.VMEM((slots, width), BF),
            pltpu.VMEM((slots, width), BF),
            pltpu.VMEM((slots, width), BF),
            pltpu.VMEM((RDIRECT * slots // 8, width), BF),
        ] + [dma((n,)) for n in n_sem],
        compiler_params=pltpu.CompilerParams(
            collective_id=0, has_side_effects=True, vmem_limit_bytes=60 * 1024 * 1024
        ),
    )(tokens, norm_gain.reshape(1, width), routing.T, gate_weight.T, w_gate, w_up, w_down)


def solution(mesh):
    placed = (
        P(("ep", "tp"), None),
        P(),
        P(("ep", "tp"), None, None),
        P(("ep", "tp"), None, None),
        P(("ep", "tp"), None, None),
        P(("ep", "tp"), None),
        P(("ep", "tp"), None),
    )
    return jax.shard_map(
        local, mesh=mesh, in_specs=placed, out_specs=P(("ep", "tp"), None), check_vma=False
    )
```

```python
import functools
import jax
import jax.numpy as jnp
from jax import lax
from jax.experimental import pallas as pl
from jax.experimental.pallas import tpu as pltpu
from jax.sharding import PartitionSpec as P

BF = jnp.bfloat16
F32 = jnp.float32
MESH = pl.DeviceIdType.MESH

CHUNKS = ((0, 1), (2, 3), (4,), (5,), (6,), (7,))
ORDER = (
    "S0 F0 S4 S2",
    "S3 F4 S5 C2",
    "F2 F3 S7 F5",
    "C1 S1 J2 F1",
    "C3 S6 F7 J3",
    "C5 G4 J1 F6",
    "C4 J5 G5 C0",
    "G3 J4 J0 G7",
    "G6 G2",
)
DIRECT = 2
RDIRECT = 2
SENDS = (
    "P2 P4 P1 P3",
    "P5 P7 X1 P6",
)


def flip(index, bits):
    unit = 1
    while unit <= bits:
        if bits & unit:
            index = index + unit - 2 * unit * lax.rem(lax.div(index, unit), 2)
        unit *= 2
    return index


def kernel(
    ep_count, tp_count, block,
    tok_ref, gain_ref, route_ref, gate_ref, wg_hbm, wu_hbm, wd_hbm, out_ref,
    wg, wu, wd, normed, pack, rows_in, hid, part, pair_in, cross_out, cross_in, done, back, back_x,
    w_sem, disp_s, disp_r, core_s, core_r, x_s, x_r, fwd_s, fwd_r,
    pair_s, pair_r, cross_s, cross_r, ret_s, ret_r, rx_s, rx_r,
):
    toks, width = tok_ref.shape
    ff = wg.shape[1]
    slots = ep_count * block
    unit = ep_count // 8
    me_e = lax.axis_index("ep")
    me_t = lax.axis_index("tp")
    partner = {"tp": flip(me_t, 1)}
    across = {"tp": flip(me_t, 2)}
    peer = [{"ep": flip(me_e, d)} for d in range(ep_count)]
    direct, r_direct = DIRECT * unit, RDIRECT * unit
    far_side = [across] + [
        {"ep": flip(me_e, d), "tp": flip(me_t, 2)} for d in range(1, max(direct, r_direct))
    ]

    w_copies = [
        pltpu.make_async_copy(src.at[0], dst, w_sem.at[i])
        for i, (src, dst) in enumerate(((wg_hbm, wg), (wu_hbm, wu), (wd_hbm, wd)))
    ]
    barrier = pltpu.get_barrier_semaphore()
    others = peer[1:] + [partner] + far_side
    for dev in others:
        pl.semaphore_signal(barrier, inc=1, device_id=dev, device_id_type=MESH)
    for c in w_copies:
        c.start()

    values = tok_ref[...].astype(F32)
    scale = lax.rsqrt(jnp.mean(values * values, axis=-1, keepdims=True) + 1e-06)
    normed[...] = (values * scale * gain_ref[...]).astype(BF)

    shift = tp_count.bit_length() - 1
    group = jnp.bitwise_xor(jnp.right_shift(route_ref[0:1, :], shift), me_e)
    in_group = (group == lax.broadcasted_iota(jnp.int32, (ep_count, toks), 0)).astype(F32)
    before = lax.broadcasted_iota(jnp.int32, (toks, toks), 0) < lax.broadcasted_iota(
        jnp.int32, (toks, toks), 1
    )
    ranks = jnp.dot(
        in_group.astype(BF), before.astype(F32).astype(BF), preferred_element_type=F32
    )
    rank = jnp.sum(ranks * in_group, axis=0, keepdims=True).astype(jnp.int32)
    slot = group * block + rank
    packing = slot == lax.broadcasted_iota(jnp.int32, (slots, toks), 0)
    packs = packing.astype(F32).astype(BF)
    step = min(slots, 128)
    for s in range(0, slots, step):
        pack[s : s + step, :width] = jnp.dot(
            packs[s : s + step, :], normed[...], preferred_element_type=F32
        ).astype(BF)
    lane = lax.broadcasted_iota(jnp.int32, (slots, 128), 1)
    weight = jnp.zeros((slots, 128), F32)
    for j in range(tp_count):
        one = jnp.zeros((1, toks), F32)
        for k in range(route_ref.shape[0]):
            hit = jnp.bitwise_and(route_ref[k : k + 1, :], tp_count - 1) == j
            one = one + jnp.where(hit, gate_ref[k : k + 1, :], 0.0)
        picked = jnp.sum(jnp.where(packing, one, 0.0), axis=-1, keepdims=True)
        weight = jnp.where(jnp.bitwise_and(lane, tp_count - 1) == j, picked, weight)
    hi = weight.astype(BF).astype(F32)
    mid = (weight - hi).astype(BF).astype(F32)
    low = weight - hi - mid
    tail = jnp.where(lane < tp_count, hi, jnp.where(lane < 2 * tp_count, mid, low))
    pack[:, width:] = jnp.where(lane < 3 * tp_count, tail, 0.0).astype(BF)

    def remote(src, dst, s, r, dev):
        return pltpu.make_async_remote_copy(
            src_ref=src, dst_ref=dst, send_sem=s, recv_sem=r, device_id=dev, device_id_type=MESH
        )

    chunk_of = {}
    first, count, base = [], [], []
    for k, units in enumerate(CHUNKS):
        first.append(units[0] * unit)
        count.append(len(units) * unit)
        base.append(units[0] * unit * block)
        for d in range(first[k], first[k] + count[k]):
            chunk_of[d] = k

    def place(d, pos):
        k = chunk_of[d]
        seg = count[k] * block
        return rows_in.at[pl.ds(tp_count * base[k] + pos * seg + (d - first[k]) * block, block)]

    rows_in[0:block, :] = pack[0:block, :]
    pl.semaphore_wait(barrier, len(others))

    disp, core, xs, fwd, ret, ret_x, pair, cross = ({} for _ in range(8))

    def send_peer(d):
        disp[d] = remote(
            pack.at[pl.ds(d * block, block)], place(d, 0), disp_s.at[d], disp_r.at[d], peer[d]
        )
        disp[d].start()

    def send_across(d, dev):
        src = pack.at[pl.ds(d * block, block)] if d < direct else place(d, 0)
        xs[d] = remote(src, place(d, 1), x_s.at[d], x_r.at[d], dev)
        xs[d].start()

    def send_core(d):
        core[d] = remote(place(d, 0), place(d, 2), core_s.at[d], core_r.at[d], partner)
        core[d].start()

    send_across(0, across)
    send_core(0)
    for d in range(1, unit):
        send_peer(d)
        send_across(d, far_side[d])
    for word in " ".join(SENDS).split():
        i = int(word[1:])
        for d in range(i * unit, i * unit + unit):
            if word[0] == "P":
                send_peer(d)
            else:
                send_across(d, far_side[d])

    def spread(i):
        for d in range(i * unit, i * unit + unit):
            if d > 0:
                disp[d].wait_recv()
                if d >= direct:
                    send_across(d, across)
                send_core(d)

    def forward(i):
        for d in range(i * unit, i * unit + unit):
            xs[d].wait_recv()
            fwd[d] = remote(place(d, 1), place(d, 3), fwd_s.at[d], fwd_r.at[d], partner)
            fwd[d].start()

    def compute(k):
        for d in range(first[k], first[k] + count[k]):
            core[d].wait_recv()
            fwd[d].wait_recv()
        if not pair:
            for c in w_copies:
                c.wait()
        seg = count[k] * block
        total = tp_count * seg
        mine = pl.ds(tp_count * base[k], total)
        ends = lax.broadcasted_iota(jnp.int32, (total, 128), 1)
        own = jnp.bitwise_and(ends, tp_count - 1) == me_t
        gates = jnp.sum(
            jnp.where(own, rows_in[mine, width:].astype(F32), 0.0), axis=-1, keepdims=True
        )
        f_tile = min(ff, 256)
        for j in range(0, ff, f_tile):
            rows = rows_in[mine, :width]
            g = jnp.dot(rows, wg[:, j : j + f_tile], preferred_element_type=F32)
            u = jnp.dot(rows, wu[:, j : j + f_tile], preferred_element_type=F32)
            hid[0:total, j : j + f_tile] = (g / (1.0 + jnp.exp(-g)) * u).astype(BF)
        d_tile = min(width, 512)
        for j in range(0, width, d_tile):
            y = jnp.dot(hid[0:total, :], wd[:, j : j + d_tile], preferred_element_type=F32)
            part[mine, j : j + d_tile] = (y * gates).astype(BF)
        pair[k] = remote(
            part.at[pl.ds(tp_count * base[k] + 2 * seg, 2 * seg)],
            pair_in.at[pl.ds(2 * base[k], 2 * seg)], pair_s.at[k], pair_r.at[k], partner,
        )
        pair[k].start()

    def give_block(d):
        ret[d] = remote(
            done.at[pl.ds(d * block, block)], back.at[pl.ds(d * block, block)],
            ret_s.at[d], ret_r.at[d], peer[d],
        )
        ret[d].start()

    def join(k):
        pair[k].wait_recv()
        seg = count[k] * block
        b, p = base[k], tp_count * base[k]
        cross_out[b : b + seg, :] = (
            part[p + seg : p + 2 * seg, :].astype(F32)
            + pair_in[2 * b + seg : 2 * b + 2 * seg, :].astype(F32)
        ).astype(BF)
        if first[k] >= r_direct:
            for d in range(first[k], first[k] + count[k]):
                cross[d] = remote(
                    cross_out.at[pl.ds(d * block, block)], cross_in.at[pl.ds(d * block, block)],
                    cross_s.at[d], cross_r.at[d], across,
                )
                cross[d].start()
            return
        for d in range(first[k], first[k] + count[k]):
            ret_x[d] = remote(
                cross_out.at[pl.ds(d * block, block)], back_x.at[pl.ds(d * block, block)],
                rx_s.at[d], rx_r.at[d], far_side[d],
            )
            ret_x[d].start()
        total = (
            part[p : p + seg, :].astype(F32) + pair_in[2 * b : 2 * b + seg, :].astype(F32)
        ).astype(BF)
        done[b : b + seg, :] = total
        for d in range(first[k], first[k] + count[k]):
            if d == 0:
                back[0:block, :] = total[0:block, :]
            else:
                give_block(d)

    def give(i):
        for d in range(i * unit, i * unit + unit):
            cross[d].wait_recv()
            k = chunk_of[d]
            b, p = d * block, tp_count * base[k] + (d - first[k]) * block
            q = 2 * base[k] + (d - first[k]) * block
            done[b : b + block, :] = (
                part[p : p + block, :].astype(F32)
                + pair_in[q : q + block, :].astype(F32)
                + cross_in[b : b + block, :].astype(F32)
            ).astype(BF)
            give_block(d)

    step_of = {"S": spread, "F": forward, "C": compute, "J": join, "G": give}
    for word in " ".join(ORDER).split():
        step_of[word[0]](int(word[1:]))

    for d in sorted(ret):
        ret[d].wait_recv()
    for d in sorted(ret_x):
        ret_x[d].wait_recv()
    unpack = packing.astype(F32).T.astype(BF)
    total = jnp.dot(unpack, back[...], preferred_element_type=F32)
    total = total + jnp.dot(
        unpack[:, : r_direct * block], back_x[...], preferred_element_type=F32
    )
    out_ref[...] = total.astype(BF)
    for group_of in (disp, core, xs, fwd, pair, cross, ret, ret_x):
        for c in group_of.values():
            c.wait_send()


def local(tokens, norm_gain, w_gate, w_up, w_down, routing, gate_weight):
    toks, width = tokens.shape
    ff = w_gate.shape[2]
    ep_count = lax.axis_size("ep")
    tp_count = lax.axis_size("tp")
    assert tp_count == 4 and ep_count % 8 == 0
    cap = toks // ep_count
    block = -(-cap // 16) * 16
    slots = ep_count * block
    wide = width + 128
    most = tp_count * block * (ep_count // 8) * max(len(units) for units in CHUNKS)
    vm = pl.BlockSpec(memory_space=pltpu.VMEM)
    hbm = pl.BlockSpec(memory_space=pl.ANY)
    dma = pltpu.SemaphoreType.DMA
    n_sem = [3] + [ep_count] * 8 + [len(CHUNKS)] * 2 + [ep_count] * 6
    return pl.pallas_call(
        functools.partial(kernel, ep_count, tp_count, block),
        out_shape=jax.ShapeDtypeStruct((toks, width), BF),
        in_specs=[vm] * 4 + [hbm] * 3,
        out_specs=vm,
        scratch_shapes=[
            pltpu.VMEM((width, ff), BF),
            pltpu.VMEM((width, ff), BF),
            pltpu.VMEM((ff, width), BF),
            pltpu.VMEM((toks, width), BF),
            pltpu.VMEM((slots, wide), BF),
            pltpu.VMEM((tp_count * slots, wide), BF),
            pltpu.VMEM((most, ff), BF),
            pltpu.VMEM((tp_count * slots, width), BF),
            pltpu.VMEM((2 * slots, width), BF),
            pltpu.VMEM((slots, width), BF),
            pltpu.VMEM((slots, width), BF),
            pltpu.VMEM((slots, width), BF),
            pltpu.VMEM((slots, width), BF),
            pltpu.VMEM((RDIRECT * slots // 8, width), BF),
        ] + [dma((n,)) for n in n_sem],
        compiler_params=pltpu.CompilerParams(
            collective_id=0, has_side_effects=True, vmem_limit_bytes=60 * 1024 * 1024
        ),
    )(tokens, norm_gain.reshape(1, width), routing.T, gate_weight.T, w_gate, w_up, w_down)


def solution(mesh):
    placed = (
        P(("ep", "tp"), None),
        P(),
        P(("ep", "tp"), None, None),
        P(("ep", "tp"), None, None),
        P(("ep", "tp"), None, None),
        P(("ep", "tp"), None),
        P(("ep", "tp"), None),
    )
    return jax.shard_map(
        local, mesh=mesh, in_specs=placed, out_specs=P(("ep", "tp"), None), check_vma=False
    )
```
